256 devices in a mesh: rep: 2 (over z_hi), fs: 16 (over z_lo, y), tp: 8 (over x, core).
Axes of the slice: x: 4, y: 4, z: 8 (z_hi: 2, z_lo: 4; z = z_hi * 4 + z_lo), core: 2. Of those that a mesh axis runs over, the one named last changes fastest.
Arguments:
- activations: bfloat16 [12288, 2048], P(('rep', 'fs'), 'tp'), may hold values from -16 to 16
- norm_gain: float32 [2048], replicated, may hold values from 0.1 to 1.9
- query_weight: bfloat16 [2048, 512], P('fs', 'tp'), may hold values from -0.125 to 0.125
- key_weight: bfloat16 [2048, 512], P('fs', 'tp'), may hold values from -0.125 to 0.125
- value_weight: bfloat16 [2048, 512], P('fs', 'tp'), may hold values from -0.125 to 0.125
- gate_weight: bfloat16 [2048, 512], P('fs', 'tp'), may hold values from -0.125 to 0.125
- out_weight: bfloat16 [512, 2048], P('tp', 'fs'), may hold values from -0.25 to 0.25
- mlp_gain: float32 [2048], replicated, may hold values from 0.1 to 1.9
- up_weight: bfloat16 [2048, 8192], P('fs', 'tp'), may hold values from -0.125 to 0.125
- down_weight: bfloat16 [8192, 2048], P('tp', 'fs'), may hold values from -0.0625 to 0.0625
Outputs:
- layer_out: bfloat16 [12288, 2048], P(('rep', 'fs'), 'tp')
The draws below stay inside these ranges and needn't reach their ends.
All inputs are finite; a program needn't handle non-finite values.
Results may differ from the reference program's by a relative error of at most 0.012.
Values may be sent and summed in bfloat16 or wider, within the bound.
No kernel may reach another device: no remote copies, remote signals or barrier semaphores. Data moves between devices by JAX's collectives and lax.ppermute only.
A program may use at most 64 MiB of HBM per device.

```python
import math
import jax
import jax.numpy as jnp
from jax import lax

D = 2048
FF = 8192
HEADS = 8
HEAD_DIM = 64
BLOCK = 64
SEQ_LEN = 128
TOKENS = 12288
N_TP = 8


def draw_activations(key, part):
    key_base, key_column, key_row = jax.random.split(jax.random.fold_in(key, 11), 3)
    column_index = jnp.arange(D, dtype=jnp.float32)
    column_scale = jnp.power(3.0, column_index / (D - 1)) * jnp.exp(jax.random.uniform(key_column, (D,), jnp.float32, -0.35, 0.35))
    base_draw = jax.random.normal(key_base, (TOKENS, D), jnp.float32)
    row_scale = jnp.exp(jax.random.uniform(key_row, (TOKENS, 1), jnp.float32, 0.0, math.log(4.0)))
    return jnp.clip(0.5 * base_draw * row_scale * column_scale[None, :], -16.0, 16.0).astype(jnp.bfloat16)


def level_of(key, shape, cuts, least, largest):
    loudness = 1.0
    for dim, shards_of in cuts:
        steps = jax.random.uniform(jax.random.fold_in(jax.random.fold_in(key, 6), dim), (shards_of,), jnp.float32, least / len(cuts), largest / len(cuts))
        loudness = loudness * jnp.repeat(jnp.exp(steps), shape[dim] // shards_of).reshape((-1,) + (1,) * (len(shape) - 1 - dim))
    return loudness


def noise(key, extent, scale, bound, cuts=(), kind=jnp.bfloat16):
    factor_of = level_of(key, extent, cuts, -0.22, 0.18) if cuts else 1.0
    values = jax.random.normal(key, extent, jnp.float32) * scale * factor_of
    return jnp.minimum(jnp.maximum(values, -bound), bound).astype(kind)


def setup_inputs(seed: int = 0) -> dict:
    streams_of = jax.random.split(jax.random.key(seed), 11)
    return {
        "activations": draw_activations(jax.random.fold_in(streams_of[10], 71), 0),
        "norm_gain": jnp.clip(1.0 + 0.18 * jax.random.normal(streams_of[1], (D,), jnp.float32), 0.1, 1.9),
        "query_weight": noise(streams_of[2], (D, HEADS * HEAD_DIM), D ** -0.5, 0.125, ((0, 16), (1, 8))),
        "key_weight": noise(streams_of[3], (D, HEADS * HEAD_DIM), D ** -0.5, 0.125, ((0, 16), (1, 8))),
        "value_weight": noise(streams_of[4], (D, HEADS * HEAD_DIM), D ** -0.5, 0.125, ((0, 16), (1, 8))),
        "gate_weight": noise(streams_of[5], (D, HEADS * HEAD_DIM), D ** -0.5, 0.125, ((0, 16), (1, 8))),
        "out_weight": noise(streams_of[6], (HEADS * HEAD_DIM, D), (HEADS * HEAD_DIM) ** -0.5, 0.25, ((0, 8), (1, 16))),
        "mlp_gain": jnp.clip(1.0 + 0.18 * jax.random.normal(streams_of[7], (D,), jnp.float32), 0.1, 1.9),
        "up_weight": noise(streams_of[8], (D, FF), D ** -0.5, 0.125, ((0, 16), (1, 8))),
        "down_weight": noise(streams_of[9], (FF, D), FF ** -0.5, 0.0625, ((0, 8), (1, 16))),
    }


EPSILON = 1e-06

def rms_norm(rows, gain):
    floats = rows.astype(jnp.float32)
    scaled = floats * lax.rsqrt(lax.optimization_barrier(jnp.mean(floats * floats, axis=-1, keepdims=True)) + EPSILON)
    return (scaled * gain.astype(jnp.float32)).astype(jnp.bfloat16)

def rotate(raw, cosine, sine, seqs, heads):
    half = HEAD_DIM // 2
    shaped = raw.reshape(seqs, SEQ_LEN, heads, HEAD_DIM)
    first, second = (shaped[..., :half], shaped[..., half:])
    return jnp.concatenate([first * cosine - second * sine, second * cosine + first * sine], axis=-1)

def retain(query_raw, key_raw, value_rows, gate_rows, first_head):
    tokens = query_raw.shape[0]
    heads = query_raw.shape[1] // HEAD_DIM
    seqs = tokens // SEQ_LEN
    blocks = SEQ_LEN // BLOCK
    half = HEAD_DIM // 2
    position = jnp.arange(SEQ_LEN, dtype=jnp.float32)
    freqs = 10000.0 ** (-jnp.arange(half, dtype=jnp.float32) / half)
    angle = position[:, None] * freqs[None, :]
    cosine = jnp.cos(angle)[:, None, :]
    sine = jnp.sin(angle)[:, None, :]
    shape_five = (seqs, blocks, BLOCK, heads, HEAD_DIM)
    queries = rotate(query_raw, cosine, sine, seqs, heads).astype(jnp.bfloat16).reshape(shape_five)
    key_block = (rotate(key_raw, cosine, sine, seqs, heads) * HEAD_DIM ** (-0.5)).astype(jnp.bfloat16).reshape(shape_five)
    value_block = value_rows.reshape(shape_five)
    head_index = first_head + jnp.arange(heads, dtype=jnp.float32)
    exponent = 5.0 + 4.0 * head_index / (HEADS - 1)
    log_gamma = jnp.log(1.0 - jnp.power(2.0, -exponent))
    offsets = jnp.arange(BLOCK, dtype=jnp.float32)
    distance = offsets[:, None] - offsets[None, :]
    decay_mask = jnp.where(distance[None] >= 0, jnp.exp(jnp.maximum(distance, 0.0)[None] * log_gamma[:, None, None]), 0.0)
    scores = jnp.einsum('snbhd,snchd->snhbc', queries.astype(jnp.float32), key_block.astype(jnp.float32))
    weights = (scores * decay_mask[None, None]).astype(jnp.bfloat16)
    inner = jnp.einsum('snhbc,snchd->snbhd', weights.astype(jnp.float32), value_block.astype(jnp.float32))
    query_decay = queries.astype(jnp.float32) * jnp.exp((offsets + 1.0)[:, None] * log_gamma[None, :])[:, :, None]
    key_decay = key_block.astype(jnp.float32) * jnp.exp((BLOCK - 1.0 - offsets)[:, None] * log_gamma[None, :])[:, :, None]
    block_decay = jnp.exp(BLOCK * log_gamma)[None, :, None, None]

    def advance(state, inputs):
        query_now, key_now, value_now = inputs
        carried = jnp.einsum('sbhd,shde->sbhe', query_now, state, precision=lax.Precision.HIGHEST)
        state = state * block_decay + jnp.einsum('sbhd,sbhe->shde', key_now, value_now, precision=lax.Precision.HIGHEST)
        return (state, carried)
    initial = jnp.zeros((seqs, heads, HEAD_DIM, HEAD_DIM), jnp.float32)
    _, cross = lax.scan(advance, initial, (jnp.moveaxis(query_decay, 1, 0), jnp.moveaxis(key_decay, 1, 0), jnp.moveaxis(value_block.astype(jnp.float32), 1, 0)))
    mixed = (inner + jnp.moveaxis(cross, 0, 1)).reshape(tokens, heads, HEAD_DIM)
    centred = mixed - lax.optimization_barrier(jnp.mean(mixed, axis=-1, keepdims=True))
    normed = centred * lax.rsqrt(lax.optimization_barrier(jnp.mean(centred * centred, axis=-1, keepdims=True)) + EPSILON)
    gated = normed * jax.nn.silu(gate_rows.reshape(tokens, heads, HEAD_DIM))
    return gated.reshape(tokens, heads * HEAD_DIM).astype(jnp.bfloat16)

def reference(activations, norm_gain, query_weight, key_weight, value_weight, gate_weight, out_weight, mlp_gain, up_weight, down_weight):
    normed = rms_norm(activations, norm_gain)
    query_raw = jnp.dot(normed, query_weight, preferred_element_type=jnp.float32)
    key_raw = jnp.dot(normed, key_weight, preferred_element_type=jnp.float32)
    value_rows = jnp.dot(normed, value_weight, preferred_element_type=jnp.float32).astype(jnp.bfloat16)
    gate_rows = jnp.dot(normed, gate_weight, preferred_element_type=jnp.float32)
    retained = retain(query_raw, key_raw, value_rows, gate_rows, 0.0)
    branch = jnp.dot(retained, out_weight, preferred_element_type=jnp.float32)
    middle = (activations.astype(jnp.float32) + branch).astype(jnp.bfloat16)
    second = rms_norm(middle, mlp_gain)
    hidden = jnp.square(jax.nn.relu(jnp.dot(second, up_weight, preferred_element_type=jnp.float32))).astype(jnp.bfloat16)
    group_width = FF // N_TP
    hidden_parts = jnp.moveaxis(hidden.reshape(hidden.shape[0], N_TP, group_width), 1, 0)
    down_parts = down_weight.reshape(N_TP, group_width, D)

    def accumulate(running, inputs):
        part_rows, part_weight = inputs
        rounded = lax.optimization_barrier(jnp.dot(part_rows, part_weight, preferred_element_type=jnp.float32).astype(jnp.bfloat16))
        return (running + rounded.astype(jnp.float32), None)
    summed, _ = lax.scan(accumulate, jnp.zeros((hidden.shape[0], D), jnp.float32), (hidden_parts, down_parts))
    return (middle.astype(jnp.float32) + summed).astype(jnp.bfloat16)
```

```python
import jax
import jax.numpy as jnp
import numpy as np
from jax import lax
from jax.experimental import pallas as pl
from jax.experimental.pallas import tpu as pltpu
from jax.sharding import PartitionSpec as P

HEADS = 8
HEAD_DIM = 64
SEQ_LEN = 128
D = 2048
CHUNKS = 16
LANES = 128
EPSILON = 1e-06


F32 = jnp.float32
BF16 = jnp.bfloat16
VMEM = pl.BlockSpec(memory_space=pltpu.VMEM)
SMEM = pl.BlockSpec(memory_space=pltpu.SMEM)


def along_x(v, steps, swap=0):
    pairs = [(i, ((i // 2 + steps) % 4) * 2 + ((i % 2) ^ swap)) for i in range(8)]
    return lax.ppermute(v, "tp", pairs)


def along_z(v, steps):
    pairs = [(i, ((i // 4 + steps) % 8) * 4 + i % 4) for i in range(32)]
    return lax.ppermute(v, ("rep", "fs"), pairs)


def along_y(v, steps):
    pairs = [(i, (i // 4) * 4 + (i % 4 + steps) % 4) for i in range(16)]
    return lax.ppermute(v, "fs", pairs)


def call(kernel, out_shapes, args, scratch=(), limit=24):
    return pl.pallas_call(
        kernel,
        out_shape=out_shapes,
        in_specs=[SMEM] + [VMEM] * (len(args) - 1),
        out_specs=[VMEM] * len(out_shapes),
        scratch_shapes=list(scratch),
        compiler_params=pltpu.CompilerParams(vmem_limit_bytes=limit << 20),
    )(*args)


def place(s_ref):
    return s_ref[0], s_ref[1], s_ref[2], s_ref[3]


def chunk_of(z, y, kz, ky):
    return ((z - kz) & 3) * 4 + ((y - ky) & 3)


def retain_kernel(
    s_ref,
    x00, x01, x10, x11, x20, x21, x30, x31,
    w0, w1, w2, w3,
    gain_ref, cos_ref, sin_ref,
    x_ref, kept_ref,
    normed, weights,
):
    z, y, x, c = place(s_ref)
    blocks = ((0, 0, x00), (0, 1, x01), (1, 0, x10), (1, 1, x11),
              (2, 0, x20), (2, 1, x21), (3, 0, x30), (3, 1, x31))
    rows = x00.shape[0]
    squares = jnp.zeros((rows, LANES), F32)
    for k, other, ref in blocks:
        group = ((x - k) & 3) * 2 + (c ^ other)
        for half in range(2):
            v = ref[:, half * LANES : (half + 1) * LANES]
            x_ref[2 * group + half] = v
            f = v.astype(F32)
            squares += f * f
    inverse = lax.rsqrt(jnp.sum(squares, axis=-1, keepdims=True) / D + EPSILON)
    for ky, w in enumerate((w0, w1, w2, w3)):
        for kz in range(4):
            at = (ky * 4 + kz) * LANES
            chunk = chunk_of(z, y, kz, ky)
            scaled = x_ref[chunk].astype(F32) * inverse * gain_ref[chunk]
            normed[:, at : at + LANES] = scaled.astype(BF16)
            b = w[kz]
            weights[0:128, at : at + LANES] = b[0:128]
            weights[128:160, at : at + LANES] = b[32:64]
            weights[160:192, at : at + LANES] = b[0:32]
            weights[192:224, at : at + LANES] = b[96:128]
            weights[224:256, at : at + LANES] = b[64:96]
            weights[256:384, at : at + LANES] = b[128:256]
    projected = lax.dot_general(
        normed[...], weights[...], (((1,), (1,)), ((), ())), preferred_element_type=F32
    )
    head = (x * 2 + c).astype(F32)
    exponent = 5.0 + 4.0 * jnp.full((SEQ_LEN, SEQ_LEN), head, F32) / (HEADS - 1)
    log_gamma = jnp.log(1.0 - jnp.exp2(-exponent))
    at_row = lax.broadcasted_iota(jnp.int32, (SEQ_LEN, SEQ_LEN), 0)
    at_col = lax.broadcasted_iota(jnp.int32, (SEQ_LEN, SEQ_LEN), 1)
    distance = (at_row - at_col).astype(F32)
    decay = jnp.where(distance >= 0, jnp.exp(jnp.maximum(distance, 0.0) * log_gamma), 0.0)
    lane = lax.broadcasted_iota(jnp.int32, (1, LANES), 1)
    scale = jnp.where(lane < HEAD_DIM, 1.0, HEAD_DIM**-0.5).astype(F32)
    kept = []
    for s in range(rows // SEQ_LEN):
        part = projected[s * SEQ_LEN : (s + 1) * SEQ_LEN]
        turned = part[:, 0:128] * cos_ref[...] + part[:, 128:256] * sin_ref[...]
        turned = (turned * scale).astype(BF16)
        q, key = turned[:, :HEAD_DIM], turned[:, HEAD_DIM:]
        value = part[:, 256:320].astype(BF16)
        gate = part[:, 320:384]
        scores = lax.dot_general(q, key, (((1,), (1,)), ((), ())), preferred_element_type=F32)
        mixed = jnp.dot((scores * decay).astype(BF16), value, preferred_element_type=F32)
        centred = mixed - jnp.mean(mixed, axis=-1, keepdims=True)
        spread = jnp.mean(centred * centred, axis=-1, keepdims=True)
        kept.append(
            (centred * lax.rsqrt(spread + EPSILON) * (gate * jax.nn.sigmoid(gate))).astype(BF16)
        )
    kept = jnp.concatenate(kept, axis=0)
    kept_ref[...] = jnp.concatenate([kept[: rows // 2], kept[rows // 2 :]], axis=1)


def middle_kernel(
    s_ref,
    r00, r01, r10, r11, r20, r21, r30, r31,
    o00, o01, o10, o11, o20, o21, o30, o31,
    x_ref, gain_ref,
    second_ref, own_ref,
    kept, middle,
):
    z, y, x, c = place(s_ref)
    rows = x_ref.shape[1]
    for n, r in enumerate((r00, r01, r10, r11, r20, r21, r30, r31)):
        v = r[...]
        at = n * HEAD_DIM
        kept[0 : rows // 2, at : at + HEAD_DIM] = v[:, :HEAD_DIM]
        kept[rows // 2 :, at : at + HEAD_DIM] = v[:, HEAD_DIM:]
    outs = (o00, o01, o10, o11, o20, o21, o30, o31)
    left = kept[...]
    squares = jnp.zeros((rows, LANES), F32)
    for n in range(0, CHUNKS, 2):
        right = jnp.concatenate(
            [jnp.concatenate([o[n], o[n + 1]], axis=1) for o in outs], axis=0
        )
        mix = jnp.dot(left, right, preferred_element_type=F32)
        for half in range(2):
            ky, kz = divmod(n + half, 4)
            base = x_ref[chunk_of(z, y, kz, ky)].astype(F32)
            m = (base + mix[:, half * LANES : (half + 1) * LANES]).astype(BF16)
            middle[n + half] = m
            f = m.astype(F32)
            squares += f * f
    inverse = lax.rsqrt(jnp.sum(squares, axis=-1, keepdims=True) / D + EPSILON)
    for n in range(CHUNKS):
        ky, kz = divmod(n, 4)
        scaled = middle[n].astype(F32) * inverse * gain_ref[chunk_of(z, y, kz, ky)]
        second_ref[:, n * LANES : (n + 1) * LANES] = scaled.astype(BF16)
    for half in range(2):
        chunk = (x * 2 + c) * 2 + half
        own_ref[half] = middle[((y - chunk) & 3) * 4 + ((z - (chunk >> 2)) & 3)]


def up_kernel(s_ref, second_ref, u0, u1, u2a, u2b, u3, hidden_ref):
    part = u2a.shape[0]
    for n in range(0, hidden_ref.shape[1], 256):
        cols = slice(n, n + 256)
        total = jnp.dot(second_ref[:, 0:512], u0[:, cols], preferred_element_type=F32)
        total += jnp.dot(second_ref[:, 512:1024], u1[:, cols], preferred_element_type=F32)
        total += jnp.dot(second_ref[:, 1536:2048], u3[:, cols], preferred_element_type=F32)
        total += jnp.dot(second_ref[:, 1024 : 1024 + part], u2a[:, cols], preferred_element_type=F32)
        total += jnp.dot(second_ref[:, 1024 + part : 1536], u2b[:, cols], preferred_element_type=F32)
        hidden_ref[:, cols] = jnp.square(jnp.maximum(total, 0.0)).astype(BF16)


def down_kernel(
    s_ref, hidden_ref, d0, d1, d2a, d2b, d3,
    p00, p01, p02, p03, p10, p11, p12, p13,
    parts,
):
    z, y, x, c = place(s_ref)
    left = hidden_ref[...]
    halves = (
        (0, 0, d0[0], d0[1]), (0, 2, d0[2], d0[3]),
        (1, 0, d1[0], d1[1]), (1, 2, d1[2], d1[3]),
        (3, 0, d3[0], d3[1]), (3, 2, d3[2], d3[3]),
        (2, 0, d2a[0], d2a[1]), (2, 2, d2b[0], d2b[1]),
    )
    for kz, ky, first, later in halves:
        out = jnp.dot(left, jnp.concatenate([first, later], axis=1), preferred_element_type=F32)
        for n in range(2):
            at = (y - ky - n) & 3
            target = (z - kz - x) & 3
            parts[(((at >> 1) ^ c) * 4 + target) * 2 + (at & 1)] = out[
                :, n * LANES : (n + 1) * LANES
            ].astype(BF16)
    for n, p in enumerate((p00, p01, p02, p03, p10, p11, p12, p13)):
        p[0] = parts[2 * n]
        p[1] = parts[2 * n + 1]


def tables():
    half = HEAD_DIM // 2
    position = np.arange(SEQ_LEN, dtype=np.float32)
    freqs = np.float32(10000.0) ** (-np.arange(half, dtype=np.float32) / np.float32(half))
    angle = position[:, None] * freqs[None, :]
    cosine, sine = np.cos(angle), np.sin(angle)
    return (
        np.concatenate([cosine] * 4, axis=1).astype(np.float32),
        np.concatenate([-sine, sine, -sine, sine], axis=1).astype(np.float32),
    )


def local(
    activations, norm_gain, query_weight, key_weight, value_weight, gate_weight,
    out_weight, mlp_gain, up_weight, down_weight,
):
    rows = activations.shape[0]
    fs, tp = lax.axis_index("fs"), lax.axis_index("tp")
    spot = jnp.stack([fs // 4, fs % 4, tp // 2, tp % 2]).astype(jnp.int32)
    cosine, sine = tables()

    xs = {(0, 0): activations}
    xs[1, 0] = along_x(activations, 1)
    xs[3, 0] = along_x(activations, -1)
    xs[2, 0] = along_x(activations, 2)
    for k in range(4):
        xs[k, 1] = along_x(xs[k, 0], 0, 1)

    small = jnp.concatenate(
        [query_weight.T, key_weight.T, value_weight.T, gate_weight.T, out_weight], axis=0
    )
    line = jnp.stack([small, along_z(small, 1), along_z(small, 2), along_z(small, -1)])
    small_by_y = [line, along_y(line, 1), along_y(line, 2), along_y(line, -1)]

    up_line = jnp.concatenate(
        [up_weight, along_z(up_weight, 1), along_z(up_weight, 2), along_z(up_weight, -1)]
    )
    down_line = jnp.stack(
        [down_weight, along_y(down_weight, 1), along_y(down_weight, 2), along_y(down_weight, -1)]
    )
    up_1, up_3 = along_y(up_line, 1), along_y(up_line, -1)
    down_1, down_3 = along_z(down_line, 1), along_z(down_line, -1)
    half = up_line.shape[0] // 2
    up_2a, up_2b = along_y(up_1[:half], 1), along_y(up_3[half:], -1)
    down_2a, down_2b = along_z(down_1[:2], 1), along_z(down_3[2:], -1)

    order = [(k, other) for k in range(4) for other in range(2)]
    x_all, kept = call(
        retain_kernel,
        (
            jax.ShapeDtypeStruct((CHUNKS, rows, LANES), BF16),
            jax.ShapeDtypeStruct((rows // 2, LANES), BF16),
        ),
        [spot]
        + [xs[at] for at in order]
        + small_by_y
        + [norm_gain.reshape(CHUNKS, 1, LANES), jnp.asarray(cosine), jnp.asarray(sine)],
        [pltpu.VMEM((rows, D), BF16), pltpu.VMEM((384, D), BF16)],
    )

    outs = {(0, 0): jnp.concatenate([b[:, 256:] for b in small_by_y], axis=0)}
    keeps = {(0, 0): kept}
    for held in (outs, keeps):
        held[1, 0] = along_x(held[0, 0], 1)
        held[3, 0] = along_x(held[0, 0], -1)
        held[2, 0] = along_x(held[0, 0], 2)
        for k in range(4):
            held[k, 1] = along_x(held[k, 0], 0, 1)

    second, own = call(
        middle_kernel,
        (
            jax.ShapeDtypeStruct((rows, D), BF16),
            jax.ShapeDtypeStruct((2, rows, LANES), BF16),
        ),
        [spot]
        + [keeps[at] for at in order]
        + [outs[at] for at in order]
        + [x_all, mlp_gain.reshape(CHUNKS, 1, LANES)],
        [pltpu.VMEM((rows, 512), BF16), pltpu.VMEM((CHUNKS, rows, LANES), BF16)],
    )
    (hidden,) = call(
        up_kernel,
        (jax.ShapeDtypeStruct((rows, up_weight.shape[1]), BF16),),
        [spot, second, up_line, up_1, up_2a, up_2b, up_3],
    )
    parts = call(
        down_kernel,
        (jax.ShapeDtypeStruct((2, rows, LANES), BF16),) * 8,
        [spot, hidden, down_line, down_1, down_2a, down_2b, down_3],
        [pltpu.VMEM((CHUNKS, rows, LANES), BF16)],
    )
    mine, theirs = parts[:4], [along_x(p, 0, 1) for p in parts[4:]]
    pairs = [a.astype(F32) + b.astype(F32) for a, b in zip(mine, theirs)]
    total = own.astype(F32) + pairs[0]
    for k in (2, 1, 3):
        total += along_x(pairs[k].astype(BF16), k if k < 3 else -1).astype(F32)
    total = total.astype(BF16)
    return jnp.concatenate([total[0], total[1]], axis=1)


def solution(mesh):
    in_specs = (
        P(("rep", "fs"), "tp"),
        P(),
        P("fs", "tp"),
        P("fs", "tp"),
        P("fs", "tp"),
        P("fs", "tp"),
        P("tp", "fs"),
        P(),
        P("fs", "tp"),
        P("tp", "fs"),
    )
    out_specs = P(("rep", "fs"), "tp")
    return jax.shard_map(local, mesh=mesh, in_specs=in_specs, out_specs=out_specs, check_vma=False)
```

```python
import jax
import jax.numpy as jnp
import numpy as np
from jax import lax
from jax.experimental import pallas as pl
from jax.experimental.pallas import tpu as pltpu
from jax.sharding import PartitionSpec as P

HEADS = 8
HEAD_DIM = 64
SEQ_LEN = 128
D = 2048
CHUNKS = 16
LANES = 128
HALF = 512
SMALL = 320
EPSILON = 1e-06


F32 = jnp.float32
BF16 = jnp.bfloat16
VMEM = pl.BlockSpec(memory_space=pltpu.VMEM)
SMEM = pl.BlockSpec(memory_space=pltpu.SMEM)
EVERY = ("rep", "fs", "tp")


def moved(v, move):
    pairs = []
    for i in range(256):
        z, y, x, c = move(i // 32, (i // 8) % 4, (i // 2) % 4, i % 2)
        pairs.append((i, (z % 8) * 32 + (y % 4) * 8 + (x % 4) * 2 + c))
    return lax.ppermute(v, EVERY, pairs)


def along_x(v, k):
    return moved(v, lambda z, y, x, c: (z, y, x + k, c))


def other_core(v):
    return moved(v, lambda z, y, x, c: (z, y, x, 1 - c))


def turn(z, y, k, down_z):
    if not down_z:
        return z, y + k
    return z + (-2 if k == 2 and z % 2 else k), y


def first_axis(v, k):
    return moved(v, lambda z, y, x, c: (*turn(z, y, k, c == 0), x, c))


def later_axis(v, k):
    return moved(v, lambda z, y, x, c: (*turn(z, y, k, c == 1), x, c))


def call(kernel, out_shapes, args, scratch=(), limit=12, aliases=None, out_spec=VMEM, cost=None):
    return pl.pallas_call(
        kernel,
        out_shape=out_shapes,
        in_specs=[SMEM] + [VMEM] * (len(args) - 1),
        out_specs=[out_spec] * len(out_shapes),
        scratch_shapes=list(scratch),
        input_output_aliases=aliases or {},
        cost_estimate=cost,
        compiler_params=pltpu.CompilerParams(vmem_limit_bytes=limit << 20),
    )(*args)


def place(s_ref):
    return s_ref[0], s_ref[1], s_ref[2], s_ref[3]


def chunk_at(s_ref, i, j, swap):
    z, y, _, c = place(s_ref)
    straight = (c ^ swap) == 0
    kz, ky = jnp.where(straight, i, j), jnp.where(straight, j, i)
    return ((z - kz) & 3) * 4 + ((y - ky) & 3)


def spot_kernel(s_ref, out_ref):
    for n in range(4):
        out_ref[n] = s_ref[n]


def pack_kernel(s_ref, up, down, q, k, v, g, o, mine_ref, send_ref, small):
    c = s_ref[3]
    for n, ref in enumerate((q, k, v, g, o)):
        small[n * 64 : (n + 1) * 64] = ref[...]
    for ref, half in ((mine_ref, c), (send_ref, 1 - c)):
        for n in range(4):
            at = pl.multiple_of(half * HALF + n * LANES, LANES)
            ref[n * LANES : (n + 1) * LANES] = up[:, pl.ds(at, LANES)]
        ref[HALF : 2 * HALF] = down[pl.ds(pl.multiple_of(half * HALF, HALF), HALF)]
        at = pl.multiple_of(half * (SMALL // 2), SMALL // 2)
        ref[2 * HALF :] = small[pl.ds(at, SMALL // 2)]


def retain_kernel(
    s_ref,
    x00, x01, x10, x11, x20, x21, x30, x31,
    m0, m1, m2, m3, t0, t1, t2, t3,
    gain_ref, cos_ref, sin_ref,
    x_ref, kept_ref,
    raw, normed, weights,
):
    z, y, x, c = place(s_ref)
    blocks = ((0, 0, x00), (0, 1, x01), (1, 0, x10), (1, 1, x11),
              (2, 0, x20), (2, 1, x21), (3, 0, x30), (3, 1, x31))
    rows = x00.shape[0]
    squares = jnp.zeros((rows, LANES), F32)
    for k, other, ref in blocks:
        group = ((x - k) & 3) * 2 + (c ^ other)
        for half in range(2):
            v = ref[:, half * LANES : (half + 1) * LANES]
            x_ref[2 * group + half] = v
            f = v.astype(F32)
            squares += f * f
    inverse = lax.rsqrt(jnp.sum(squares, axis=-1, keepdims=True) / D + EPSILON)

    part = SMALL // 2
    for j, (m, t) in enumerate(((m0, t0), (m1, t1), (m2, t2), (m3, t3))):
        for i in range(4):
            at = pl.multiple_of(c * part, part)
            raw[chunk_at(s_ref, i, j, 0), pl.ds(at, part)] = m[0, i]
            at = pl.multiple_of((1 - c) * part, part)
            raw[chunk_at(s_ref, i, j, 1), pl.ds(at, part)] = t[i]

    def prepare(n, _):
        at = pl.ds(pl.multiple_of(n * LANES, LANES), LANES)
        scaled = x_ref[n].astype(F32) * inverse * gain_ref[n]
        normed[:, at] = scaled.astype(BF16)
        b = raw[n]
        weights[0:128, at] = b[0:128]
        weights[128:160, at] = b[32:64]
        weights[160:192, at] = b[0:32]
        weights[192:224, at] = b[96:128]
        weights[224:256, at] = b[64:96]
        weights[256:384, at] = b[128:256]
        kept_ref[pl.ds(pl.multiple_of(n * 64, 64), 64)] = b[256:320]
        return _

    lax.fori_loop(0, CHUNKS, prepare, 0)
    projected = lax.dot_general(
        normed[...], weights[...], (((1,), (1,)), ((), ())), preferred_element_type=F32
    )
    head = (x * 2 + c).astype(F32)
    exponent = 5.0 + 4.0 * jnp.full((SEQ_LEN, SEQ_LEN), head, F32) / (HEADS - 1)
    log_gamma = jnp.log(1.0 - jnp.exp2(-exponent))
    at_row = lax.broadcasted_iota(jnp.int32, (SEQ_LEN, SEQ_LEN), 0)
    at_col = lax.broadcasted_iota(jnp.int32, (SEQ_LEN, SEQ_LEN), 1)
    distance = (at_row - at_col).astype(F32)
    decay = jnp.where(distance >= 0, jnp.exp(jnp.maximum(distance, 0.0) * log_gamma), 0.0)
    lane = lax.broadcasted_iota(jnp.int32, (1, LANES), 1)
    scale = jnp.where(lane < HEAD_DIM, 1.0, HEAD_DIM**-0.5).astype(F32)
    kept = []
    for s in range(rows // SEQ_LEN):
        now = projected[s * SEQ_LEN : (s + 1) * SEQ_LEN]
        turned = now[:, 0:128] * cos_ref[...] + now[:, 128:256] * sin_ref[...]
        turned = (turned * scale).astype(BF16)
        q, key = turned[:, :HEAD_DIM], turned[:, HEAD_DIM:]
        value = now[:, 256:320].astype(BF16)
        gate = now[:, 320:384]
        scores = lax.dot_general(q, key, (((1,), (1,)), ((), ())), preferred_element_type=F32)
        mixed = jnp.dot((scores * decay).astype(BF16), value, preferred_element_type=F32)
        centred = mixed - jnp.mean(mixed, axis=-1, keepdims=True)
        spread = jnp.mean(centred * centred, axis=-1, keepdims=True)
        kept.append(
            (centred * lax.rsqrt(spread + EPSILON) * (gate * jax.nn.sigmoid(gate))).astype(BF16)
        )
    kept = jnp.concatenate(kept, axis=0)
    kept_ref[CHUNKS * 64 :] = jnp.concatenate([kept[: rows // 2], kept[rows // 2 :]], axis=1)


def middle_kernel(
    s_ref,
    b00, b01, b10, b11, b20, b21, b30, b31,
    x_ref, gain_ref,
    second_ref, own_ref,
    kept, squares,
):
    z, y, x, c = place(s_ref)
    rows = x_ref.shape[1]
    bundles = (b00, b01, b10, b11, b20, b21, b30, b31)
    for n, b in enumerate(bundles):
        v = b[CHUNKS * 64 :]
        at = n * HEAD_DIM
        kept[0 : rows // 2, at : at + HEAD_DIM] = v[:, :HEAD_DIM]
        kept[rows // 2 :, at : at + HEAD_DIM] = v[:, HEAD_DIM:]
    squares[...] = jnp.zeros((rows, LANES), F32)

    def mix_pair(n, _):
        first = pl.ds(pl.multiple_of(n * 128, 128), 64)
        later = pl.ds(pl.multiple_of(n * 128 + 64, 64), 64)
        right = jnp.concatenate(
            [jnp.concatenate([b[first], b[later]], axis=1) for b in bundles], axis=0
        )
        mix = jnp.dot(kept[...], right, preferred_element_type=F32)
        for half in range(2):
            base = x_ref[2 * n + half].astype(F32)
            m = (base + mix[:, half * LANES : (half + 1) * LANES]).astype(BF16)
            second_ref[2 * n + half] = m
            f = m.astype(F32)
            squares[...] += f * f
        return _

    lax.fori_loop(0, CHUNKS // 2, mix_pair, 0)
    inverse = lax.rsqrt(jnp.sum(squares[...], axis=-1, keepdims=True) / D + EPSILON)
    for half in range(2):
        own_ref[half] = second_ref[(x * 2 + c) * 2 + half]

    def scale(n, _):
        second_ref[n] = (second_ref[n].astype(F32) * inverse * gain_ref[n]).astype(BF16)
        return _

    lax.fori_loop(0, CHUNKS, scale, 0)


def up_kernel(
    s_ref, second_ref,
    m0, m1, m2a, m2b, m3, t0, t1, t2a, t2b, t3,
    mine_ref, theirs_ref,
):
    for swap, out_ref, refs in (
        (0, mine_ref, (m0, m1, m2a, m2b, m3)),
        (1, theirs_ref, (t0, t1, t2a, t2b, t3)),
    ):
        b0, b1, b2a, b2b, b3 = refs
        blocks = (
            [(0, i, b0, i) for i in range(4)] + [(1, i, b1, i) for i in range(4)]
            + [(3, i, b3, i) for i in range(4)]
            + [(2, 0, b2a, 0), (2, 1, b2a, 1), (2, 2, b2b, 0), (2, 3, b2b, 1)]
        )
        left = jnp.concatenate(
            [second_ref[chunk_at(s_ref, i, j, swap)] for j, i, _, _ in blocks], axis=1
        )

        def columns(n, carry, out_ref=out_ref, blocks=blocks, left=left, swap=swap):
            rows = []
            for _, _, ref, at in blocks:
                b = ref.at[0, at] if swap == 0 else ref.at[at]
                rows.append(jnp.concatenate([b[2 * n], b[2 * n + 1]], axis=1))
            right = jnp.concatenate(rows, axis=0)
            total = jnp.dot(left, right, preferred_element_type=F32)
            cols = pl.ds(pl.multiple_of(n * 256, 256), 256)
            out_ref[:, cols] = jnp.square(jnp.maximum(total, 0.0)).astype(BF16)
            return carry

        lax.fori_loop(0, 2, columns, 0)


def spot_of(s_ref, i, j):
    z, y, x, c = place(s_ref)
    chunk = chunk_at(s_ref, i, j, 0)
    zz, yy = chunk >> 2, chunk & 3
    return (((yy >> 1) ^ c) * 4 + ((zz - x) & 3)) * 2 + (yy & 1)


def down_some(s_ref, left, parts, todo):
    for n in range(0, len(todo), 2):
        some = todo[n : n + 2]
        right = jnp.concatenate(
            [jnp.concatenate([b for b in mine + theirs], axis=0) for _, _, mine, theirs in some],
            axis=1,
        )
        out = jnp.dot(left, right, preferred_element_type=F32)
        for k, (i, j, _, _) in enumerate(some):
            parts[spot_of(s_ref, i, j)] = out[:, k * LANES : (k + 1) * LANES].astype(BF16)


def early_kernel(s_ref, mine_ref, theirs_ref, m0, m1, m3, t0, t1, t3, parts):
    left = jnp.concatenate([mine_ref[...], theirs_ref[...]], axis=1)
    m, t = {0: m0, 1: m1, 3: m3}, {0: t0, 1: t1, 3: t3}
    todo = []
    for i in (0, 1, 3):
        for j in (0, 1, 3):
            mine = [m[j][0, i, n] for n in range(4, 8)]
            theirs = [t[i][j, n] for n in range(4, 8)]
            todo.append((i, j, mine, theirs))
    down_some(s_ref, left, parts, todo)


def late_kernel(
    s_ref, mine_ref, theirs_ref, m0, m1, m3, t0, t1, t3, m2a, m2b, t2a, t2b, before, parts
):
    left = jnp.concatenate([mine_ref[...], theirs_ref[...]], axis=1)
    m, t = {0: m0, 1: m1, 3: m3}, {0: t0, 1: t1, 3: t3}

    def mine_of(i, j):
        if j == 2:
            ref = m2a if i < 2 else m2b
            return [ref[0, i % 2, n] for n in range(4)]
        return [m[j][0, i, n] for n in range(4, 8)]

    def theirs_of(i, j):
        if i == 2:
            ref = t2a if j < 2 else t2b
            return [ref[j % 2, n] for n in range(4)]
        return [t[i][j, n] for n in range(4, 8)]

    some = [(0, 2), (1, 2), (2, 0), (2, 1), (3, 2), (2, 3), (2, 2)]
    down_some(s_ref, left, parts, [(i, j, mine_of(i, j), theirs_of(i, j)) for i, j in some])


def tables():
    half = HEAD_DIM // 2
    position = np.arange(SEQ_LEN, dtype=np.float32)
    freqs = np.float32(10000.0) ** (-np.arange(half, dtype=np.float32) / np.float32(half))
    angle = position[:, None] * freqs[None, :]
    cosine, sine = np.cos(angle), np.sin(angle)
    return (
        np.concatenate([cosine] * 4, axis=1).astype(np.float32),
        np.concatenate([-sine, sine, -sine, sine], axis=1).astype(np.float32),
    )


def layer(
    activations, norm_gain, query_weight, key_weight, value_weight, gate_weight,
    out_weight, mlp_gain, up_weight, down_weight,
):
    rows = activations.shape[0]
    fs, tp = lax.axis_index("fs"), lax.axis_index("tp")
    spot = jnp.stack([fs >> 2, fs & 3, tp >> 1, tp & 1]).astype(jnp.int32)
    cosine, sine = tables()
    (spot,) = call(
        spot_kernel,
        (jax.ShapeDtypeStruct((4,), jnp.int32),),
        [spot],
        out_spec=SMEM,
        cost=pl.CostEstimate(flops=2000000000, bytes_accessed=0, transcendentals=0),
    )

    block = 2 * HALF + SMALL // 2
    mine, send = call(
        pack_kernel,
        (jax.ShapeDtypeStruct((block, LANES), BF16),) * 2,
        [spot, up_weight, down_weight, query_weight.T, key_weight.T, value_weight.T,
         gate_weight.T, out_weight],
        [pltpu.VMEM((SMALL, LANES), BF16)],
    )
    pair = jnp.stack([mine, other_core(send)])

    xs = {(0, 0): activations}
    for k in (1, 3, 2):
        xs[k, 0] = along_x(activations, k if k < 3 else -1)
    for k in (0, 1, 3, 2):
        xs[k, 1] = other_core(xs[k, 0])

    lines = [pair] + [first_axis(pair, k if k < 3 else -1) for k in (1, 2, 3)]
    small = jnp.stack([v[:, 2 * HALF :] for v in lines], axis=1)
    large = jnp.stack(
        [v[:, : 2 * HALF].reshape(2, 8, LANES, LANES) for v in lines], axis=1
    )
    small_m = [small] + [later_axis(small, k if k < 3 else -1) for k in (1, 2, 3)]
    small_t = [other_core(v[1]) for v in small_m]
    m0 = large
    m1, m3 = later_axis(large, 1), later_axis(large, -1)
    u2a, u2b = later_axis(m1[:, :2, :4], 1), later_axis(m3[:, 2:, :4], -1)
    d2a, d2b = later_axis(m1[:, :2, 4:], 1), later_axis(m3[:, 2:, 4:], -1)
    t0, t1, t3 = (other_core(v[1]) for v in (m0, m1, m3))
    tu2a, tu2b = other_core(u2a[1]), other_core(u2b[1])
    td2a, td2b = other_core(d2a[1]), other_core(d2b[1])

    order = [(k, other) for k in range(4) for other in range(2)]
    bundle_rows = CHUNKS * 64 + rows // 2
    x_all, bundle = call(
        retain_kernel,
        (
            jax.ShapeDtypeStruct((CHUNKS, rows, LANES), BF16),
            jax.ShapeDtypeStruct((bundle_rows, LANES), BF16),
        ),
        [spot] + [xs[at] for at in order] + small_m + small_t
        + [norm_gain.reshape(CHUNKS, 1, LANES), jnp.asarray(cosine), jnp.asarray(sine)],
        [
            pltpu.VMEM((CHUNKS, SMALL, LANES), BF16),
            pltpu.VMEM((rows, D), BF16),
            pltpu.VMEM((384, D), BF16),
        ],
    )
    bundles = {(0, 0): bundle}
    for k in (1, 3, 2):
        bundles[k, 0] = along_x(bundle, k if k < 3 else -1)
    for k in (0, 1, 3, 2):
        bundles[k, 1] = other_core(bundles[k, 0])

    second, own = call(
        middle_kernel,
        (
            jax.ShapeDtypeStruct((CHUNKS, rows, LANES), BF16),
            jax.ShapeDtypeStruct((2, rows, LANES), BF16),
        ),
        [spot] + [bundles[at] for at in order]
        + [x_all, mlp_gain.reshape(CHUNKS, 1, LANES)],
        [pltpu.VMEM((rows, 512), BF16), pltpu.VMEM((rows, LANES), F32)],
    )
    hidden = call(
        up_kernel,
        (jax.ShapeDtypeStruct((rows, HALF), BF16),) * 2,
        [spot, second, m0, m1, u2a, u2b, m3, t0, t1, tu2a, tu2b, t3],
    )
    whole = jax.ShapeDtypeStruct((CHUNKS, rows, LANES), BF16)
    (early,) = call(early_kernel, (whole,), [spot, *hidden, m0, m1, m3, t0, t1, t3])
    (parts,) = call(
        late_kernel,
        (whole,),
        [spot, *hidden, m0, m1, m3, t0, t1, t3, d2a, d2b, td2a, td2b, early],
        aliases={13: 0},
    )
    pairs = []
    for k in range(4):
        theirs = other_core(parts[8 + 2 * k : 10 + 2 * k])
        pairs.append(parts[2 * k : 2 * k + 2].astype(F32) + theirs.astype(F32))
    total = own.astype(F32) + pairs[0]
    for k in (2, 1, 3):
        total += along_x(pairs[k].astype(BF16), k if k < 3 else -1).astype(F32)
    total = total.astype(BF16)
    return jnp.concatenate([total[0], total[1]], axis=1)


def solution(mesh):
    in_specs = (
        P(("rep", "fs"), "tp"),
        P(),
        P("fs", "tp"),
        P("fs", "tp"),
        P("fs", "tp"),
        P("fs", "tp"),
        P("tp", "fs"),
        P(),
        P("fs", "tp"),
        P("tp", "fs"),
    )
    out_specs = P(("rep", "fs"), "tp")
    return jax.shard_map(layer, mesh=mesh, in_specs=in_specs, out_specs=out_specs, check_vma=False)
```
